32 devices in a mesh: ep: 8 (over z, core), tp: 4 (over y, x).
Axes of the slice: x: 2, y: 2, z: 4, core: 2. Of those that a mesh axis runs over, the one named last changes fastest.
Arguments:
- tokens: bfloat16 [512, 2048], P('ep', 'tp'), may hold values from -20 to 20
- state: float32 [512, 16, 64, 64], P('ep', 'tp'), may hold values from -1.5 to 1.5
- attn_gain: float32 [2048], replicated, may hold values from 0.1 to 1.9
- ffn_gain: float32 [2048], replicated, may hold values from 0.1 to 1.9
- w_query: bfloat16 [2048, 1024], P(None, 'tp'), may hold values from -0.125 to 0.125
- w_key: bfloat16 [2048, 1024], P(None, 'tp'), may hold values from -0.125 to 0.125
- w_value: bfloat16 [2048, 1024], P(None, 'tp'), may hold values from -0.125 to 0.125
- w_output_gate: bfloat16 [2048, 1024], P(None, 'tp'), may hold values from -0.125 to 0.125
- w_decay: bfloat16 [2048, 16], replicated, may hold values from -0.125 to 0.125
- w_beta: bfloat16 [2048, 16], replicated, may hold values from -0.125 to 0.125
- decay_rate: float32 [16], P('tp'), may hold values from 0.1 to 2
- decay_shift: float32 [16], P('tp'), may hold values from -2 to 1
- head_gain: float32 [64], replicated, may hold values from 0.1 to 1.9
- w_mix_out: bfloat16 [1024, 2048], P(None, 'tp'), may hold values from -0.1875 to 0.1875
- expert_ids: int32 [512, 2], P('ep'), may hold values from 0 to 7, all different within a row; in each aligned block of 64 rows (0 to 63, 64 to 127, ...) at most 32 rows name the same one
- expert_weights: float32 [512, 2], P('ep'), may hold values from 0.2 to 1
- w_gate: bfloat16 [8, 2048, 4096], P('ep', None, 'tp'), may hold values from -0.125 to 0.125
- w_up: bfloat16 [8, 2048, 4096], P('ep', None, 'tp'), may hold values from -0.125 to 0.125
- w_down: bfloat16 [8, 4096, 2048], P('ep', 'tp'), may hold values from -0.09375 to 0.09375
Outputs:
- layer_out: bfloat16 [512, 2048], P('ep', 'tp')
- new_state: float32 [512, 16, 64, 64], P('ep', 'tp')
The draws below stay inside these ranges and needn't reach their ends.
Inputs may be any that keep to these rules, and one draw needn't show every extreme that they name: `expert_ids`: each row names 2 different experts; within the rows of one index of ep (aligned blocks of 64 rows) no expert is named by more than 32 rows, and in some blocks one expert is named by exactly 32 rows.
All inputs are finite; a program needn't handle non-finite values.
Results may differ from the reference program's by a relative error of at most 0.013.
Values may be sent and summed in bfloat16 or wider, within the bound.
A program may use at most 64 MiB of HBM per device.

```python
import math
import jax
import jax.numpy as jnp
import numpy as np
from jax import lax

D = 2048
HEADS = 16
HEAD_DIM = 64
DN_W = 1024
FF = 4096
EXPERTS = 8
TOPK = 2
SEQS = 64
TOKENS = 512
CAP = 32
N_EP = 8
N_TP = 4


def draw_tokens(key, part):
    key_rows = jax.random.fold_in(key, 11)
    key_cols = jax.random.fold_in(key, 12)
    key_vals = jax.random.fold_in(key, 13)
    row_scale = jnp.exp(jax.random.uniform(key_rows, (TOKENS, 1), jnp.float32, math.log(0.5), math.log(2.0)))
    rising = jnp.exp(jnp.linspace(math.log(0.5), math.log(1.5), D, dtype=jnp.float32))
    rough = jnp.exp(jax.random.uniform(key_cols, (D,), jnp.float32, math.log(0.8), math.log(1.25)))
    col_scale = (rising * rough)[None, :]
    values = jnp.clip(jax.random.normal(key_vals, (TOKENS, D), jnp.float32), -4.0, 4.0)
    return (values * row_scale * col_scale).astype(jnp.bfloat16)


def steps_of(key, shape, cuts, least, top_value):
    factor_of = 1.0
    for axis_at, shards_of in cuts:
        draws = jax.random.uniform(jax.random.fold_in(jax.random.fold_in(key, 6), axis_at), (shards_of,), jnp.float32, least / len(cuts), top_value / len(cuts))
        factor_of = factor_of * jnp.repeat(jnp.exp(draws), shape[axis_at] // shards_of).reshape((-1,) + (1,) * (len(shape) - 1 - axis_at))
    return factor_of


def shared_out(own_key, own, number, rows, number_of, top, reach, slope):
    ranking = jax.random.permutation(own_key, number_of)
    crowded, usual = portions_of(number_of, rows * top, reach, slope, True), portions_of(number_of, rows * top, reach, slope, False)
    places = jnp.arange(number_of)

    def named(lengths, turn):
        used = int((lengths > 0).sum())
        fixed = max(1, used // 4)
        moved = fixed + (places - fixed + turn * (used - fixed)) % max(1, number_of - fixed)
        return jnp.zeros((number_of,), jnp.int32).at[ranking[jnp.where(places < fixed, places, moved)]].set(jnp.asarray(lengths, jnp.int32))

    lengths = jnp.where(number % 4 == 0, named(crowded, number // 4), named(usual, number - number // 4 - 1))
    mixed = jax.random.permutation(jax.random.fold_in(own, 3), number_of)
    giver, taker = mixed[0:number_of // 2 * 2:2], mixed[1:number_of // 2 * 2:2]
    room = jnp.minimum(lengths[giver] - 1, reach - lengths[taker]) // 2
    room = jnp.where((giver == ranking[0]) | (taker == ranking[0]) | (lengths[taker] == 0), 0, jnp.maximum(room, 0))
    moved = jax.random.randint(jax.random.fold_in(own, 4), (number_of // 2,), 0, 1 << 20) % (room + 1)
    lengths = lengths.at[giver].add(-moved).at[taker].add(moved)
    items = jnp.searchsorted(jnp.cumsum(lengths), jnp.arange(rows * top), side="right").astype(jnp.int32)
    grid = items.reshape(top, rows).T
    grid = grid[jax.random.permutation(jax.random.fold_in(own, 1), rows)]
    turn = jax.random.randint(jax.random.fold_in(own, 2), (rows, 1), 0, top)
    return jnp.take_along_axis(grid, (jnp.arange(top)[None, :] + turn) % top, axis=1)


def portions_of(amount, total, reach, skew, full):
    portions = [(1 << 20) // math.isqrt(grade ** skew) + 1 for grade in range(1, amount + 1)]
    largest = reach if full else min(reach, max(-(-total // amount), total * portions[0] // sum(portions)))
    least = 1 if total - largest >= amount - 1 else 0
    given, surplus = [largest] + [least] * (amount - 1), total - largest - least * (amount - 1)
    while surplus > 0:
        free = [i for i in range(1, amount) if given[i] < largest] or [i for i in range(1, amount) if given[i] < reach]
        mass, left = sum([portions[i] for i in free]), surplus
        for i in free:
            addition = min(reach - given[i], max(1, left * portions[i] // mass), surplus)
            given[i] = given[i] + addition
            surplus = surplus - addition
    return np.array(given)


def centred(key, dims, spread, most, split=(), kind=jnp.bfloat16):
    loudness = steps_of(key, dims, split, -0.22, 0.18) if split else 1.0
    values = jax.random.normal(key, dims, jnp.float32) * spread * loudness
    return jnp.minimum(jnp.maximum(values, -most), most).astype(kind)


def setup_inputs(seed: int = 0) -> dict:
    arg_keys = jax.random.split(jax.random.key(seed), 20)
    tokens = draw_tokens(jax.random.fold_in(arg_keys[19], 71), 0)
    state = centred(arg_keys[1], (TOKENS, HEADS, HEAD_DIM, HEAD_DIM), 0.3, 1.5, ((0, 8), (1, 4)), jnp.float32)
    attn_gain = jnp.clip(1.0 + 0.18 * jax.random.normal(arg_keys[2], (D,), jnp.float32), 0.1, 1.9)
    ffn_gain = jnp.clip(1.0 + 0.18 * jax.random.normal(arg_keys[3], (D,), jnp.float32), 0.1, 1.9)
    w_query = centred(arg_keys[4], (D, DN_W), D ** -0.5, 0.125, ((1, 4),))
    w_key = centred(arg_keys[5], (D, DN_W), D ** -0.5, 0.125, ((1, 4),))
    w_value = centred(arg_keys[6], (D, DN_W), D ** -0.5, 0.125, ((1, 4),))
    w_output_gate = centred(arg_keys[7], (D, DN_W), D ** -0.5, 0.125, ((1, 4),))
    w_decay = centred(arg_keys[8], (D, HEADS), D ** -0.5, 0.125)
    w_beta = centred(arg_keys[9], (D, HEADS), D ** -0.5, 0.125)
    decay_rate = jnp.clip(jnp.exp(math.log(2.0) - 2.9957323 * jax.random.uniform(arg_keys[10], (HEADS,), jnp.float32) ** steps_of(arg_keys[10], (HEADS,), ((0, 4),), -0.2, 0.2)), 0.1, 2.0)
    decay_shift = jnp.clip(-2.0 + 3.0 * jax.random.uniform(arg_keys[11], (HEADS,), jnp.float32) ** steps_of(arg_keys[11], (HEADS,), ((0, 4),), -0.2, 0.2), -2.0, 1.0)
    head_gain = jnp.clip(1.0 + 0.18 * jax.random.normal(arg_keys[12], (HEAD_DIM,), jnp.float32), 0.1, 1.9)
    w_mix_out = centred(arg_keys[13], (DN_W, D), DN_W ** -0.5, 0.1875, ((1, 4),))
    expert_ids_keys = jax.random.split(jax.random.fold_in(arg_keys[14], 1), TOKENS // SEQS)
    expert_ids_turns = jax.random.permutation(jax.random.fold_in(arg_keys[14], 3), TOKENS // SEQS)
    expert_ids = jax.vmap(lambda own, number: shared_out(jax.random.fold_in(arg_keys[14], 2), own, number, SEQS, EXPERTS, TOPK, CAP, 1))(expert_ids_keys, expert_ids_turns).reshape((TOKENS, TOPK))
    expert_weights = jnp.clip(0.2 + 0.8 * jax.random.uniform(arg_keys[15], (TOKENS, TOPK), jnp.float32) ** steps_of(arg_keys[15], (TOKENS, TOPK), ((0, 8),), -0.2, 0.2), 0.2, 1.0)
    w_gate = centred(arg_keys[16], (EXPERTS, D, FF), D ** -0.5, 0.125, ((0, 8), (2, 4)))
    w_up = centred(arg_keys[17], (EXPERTS, D, FF), D ** -0.5, 0.125, ((0, 8), (2, 4)))
    w_down = centred(arg_keys[18], (EXPERTS, FF, D), FF ** -0.5, 0.09375, ((0, 8), (1, 4)))
    return dict(tokens=tokens, state=state, attn_gain=attn_gain, ffn_gain=ffn_gain, w_query=w_query, w_key=w_key, w_value=w_value, w_output_gate=w_output_gate, w_decay=w_decay, w_beta=w_beta, decay_rate=decay_rate, decay_shift=decay_shift, head_gain=head_gain, w_mix_out=w_mix_out, expert_ids=expert_ids, expert_weights=expert_weights, w_gate=w_gate, w_up=w_up, w_down=w_down)


EPS = 1e-06

def rms_scale(values):
    return lax.rsqrt(lax.optimization_barrier(jnp.mean(values * values, axis=-1, keepdims=True)) + EPS)

def unit_norm(values):
    return values * lax.rsqrt(lax.optimization_barrier(jnp.sum(values * values, axis=-1, keepdims=True)) + EPS)

def stored(values):
    return lax.optimization_barrier(values.astype(jnp.bfloat16)).astype(jnp.float32)

def slot_tables(expert_ids, expert_weights):
    pair_count = SEQS * TOPK
    block_ids = expert_ids.reshape(N_EP, pair_count)
    one_hot = (block_ids[:, :, None] == jnp.arange(EXPERTS, dtype=jnp.int32)[None, None, :]).astype(jnp.int32)
    earlier = jnp.cumsum(one_hot, axis=1) - one_hot
    slot_rank = lax.optimization_barrier(jnp.sum(earlier * one_hot, axis=2)).astype(jnp.int32)
    block_index = jnp.arange(N_EP, dtype=jnp.int32)[:, None]
    position = (block_ids * (N_EP * CAP) + block_index * CAP + slot_rank).reshape(-1)
    token_of = (jnp.arange(TOKENS * TOPK, dtype=jnp.int32) // TOPK).astype(jnp.int32)
    table_token = jnp.zeros((EXPERTS * N_EP * CAP,), jnp.int32).at[position].set(token_of)
    table_weight = jnp.zeros((EXPERTS * N_EP * CAP,), jnp.float32).at[position].set(expert_weights.reshape(-1))
    return (table_token, table_weight)

def reference(tokens, state, attn_gain, ffn_gain, w_query, w_key, w_value, w_output_gate, w_decay, w_beta, decay_rate, decay_shift, head_gain, w_mix_out, expert_ids, expert_weights, w_gate, w_up, w_down):
    tokens_f32 = tokens.astype(jnp.float32)
    normed = (tokens_f32 * rms_scale(tokens_f32) * attn_gain).astype(jnp.bfloat16)

    def project(weight):
        return jnp.dot(normed, weight, preferred_element_type=jnp.float32)

    def by_head(values):
        return values.reshape(TOKENS, HEADS, HEAD_DIM)
    query_proj = stored(project(w_query))
    key_proj = stored(project(w_key))
    value_proj = stored(project(w_value))
    gate_proj = stored(project(w_output_gate))
    keep_rate = jnp.exp(-decay_rate * jax.nn.softplus(project(w_decay) + decay_shift))
    beta_gate = jax.nn.sigmoid(project(w_beta))
    query_head = unit_norm(jax.nn.silu(by_head(query_proj))) * HEAD_DIM ** (-0.5)
    key_head = unit_norm(jax.nn.silu(by_head(key_proj)))
    value_head = jax.nn.silu(by_head(value_proj))
    decayed = keep_rate[:, :, None, None] * state
    recalled = jnp.einsum('thd,thde->the', key_head, decayed, precision=lax.Precision.HIGHEST)
    correction = beta_gate[:, :, None] * (value_head - recalled)
    new_state = decayed + key_head[:, :, :, None] * correction[:, :, None, :]
    reading = jnp.einsum('thd,thde->the', query_head, new_state, precision=lax.Precision.HIGHEST)
    head_out = (reading * rms_scale(reading) * head_gain * jax.nn.silu(by_head(gate_proj))).astype(jnp.bfloat16)
    mixed = jnp.dot(head_out.reshape(TOKENS, DN_W), w_mix_out, preferred_element_type=jnp.float32)
    residual = (tokens_f32 + mixed).astype(jnp.bfloat16)
    residual_f32 = residual.astype(jnp.float32)
    normed_ffn = (residual_f32 * rms_scale(residual_f32) * ffn_gain).astype(jnp.bfloat16)
    table_token, table_weight = slot_tables(expert_ids, expert_weights)

    def one_expert(operands):
        token_list, gate_weight, up_weight, down_weight = operands
        inputs = normed_ffn[token_list]
        gate_sum = jnp.dot(inputs, gate_weight, preferred_element_type=jnp.float32)
        up_sum = jnp.dot(inputs, up_weight, preferred_element_type=jnp.float32)
        expert_hidden = (jax.nn.silu(gate_sum) * up_sum).astype(jnp.bfloat16)
        split_hidden = expert_hidden.reshape(N_EP * CAP, N_TP, FF // N_TP).astype(jnp.float32)
        split_down = down_weight.reshape(N_TP, FF // N_TP, D).astype(jnp.float32)
        partial_value = jnp.einsum('rjf,jfd->jrd', split_hidden, split_down).astype(jnp.bfloat16)
        return lax.optimization_barrier(jnp.sum(partial_value.astype(jnp.float32), axis=0)).astype(jnp.bfloat16)
    expert_out = lax.map(one_expert, (table_token.reshape(EXPERTS, N_EP * CAP), w_gate, w_up, w_down))
    weighted = table_weight[:, None] * expert_out.reshape(EXPERTS * N_EP * CAP, D).astype(jnp.float32)
    routed = jnp.zeros((TOKENS, D), jnp.float32).at[table_token].add(weighted)
    layer_out = (residual_f32 + routed).astype(jnp.bfloat16)
    return (layer_out, new_state)
```

```python
import functools

import jax
import jax.numpy as jnp
from jax import lax
from jax.experimental import pallas as pl
from jax.experimental.pallas import tpu as pltpu
from jax.sharding import PartitionSpec as P

EPS = 1e-06
MESH = pl.DeviceIdType.MESH
GROUPS = 2
F32 = jnp.float32
BF16 = jnp.bfloat16


def unit_norm(values):
    return values * lax.rsqrt(jnp.sum(values * values, axis=-1, keepdims=True) + EPS)


def stored(values):
    return lax.optimization_barrier(values.astype(jnp.bfloat16)).astype(jnp.float32)


def remote(src, dst, send_sem, recv_sem, where):
    return pltpu.make_async_remote_copy(
        src_ref=src, dst_ref=dst, send_sem=send_sem, recv_sem=recv_sem,
        device_id=where, device_id_type=MESH)


def tail_kernel(
    n, m,
    head_ref, tok_ref, gain_ref, disp_ref, comb_ref, weight_ref,
    mix_hbm, gate_hbm, up_hbm, down_hbm,
    out_ref,
    head_all, mix_v, gate_v, up_v, down_v, outgoing, seg, normed, hidden, part,
    arrived, result, returned, resid,
    load_sem, head_send, head_recv, disp_send, disp_recv, fwd_send, fwd_recv,
    part_send, part_recv, back_send, back_recv, local_sem,
):
    me = lax.axis_index("ep")
    tp = lax.axis_index("tp")
    cap, width = outgoing.shape[1:]
    rows = tok_ref.shape[0]
    head_width = head_ref.shape[1]
    per = n // GROUPS
    group_rows = per * cap
    tp_at = [lax.rem(tp + d, m) for d in range(m)]
    ep_up = [lax.rem(me + k, n) for k in range(n)]
    ep_down = [lax.rem(me + n - k, n) for k in range(n)]

    loads = [
        pltpu.make_async_copy(mix_hbm, mix_v, load_sem.at[0]),
        pltpu.make_async_copy(gate_hbm.at[0], gate_v, load_sem.at[1]),
        pltpu.make_async_copy(up_hbm.at[0], up_v, load_sem.at[2]),
        pltpu.make_async_copy(down_hbm.at[0], down_v, load_sem.at[3]),
    ]
    loads[0].start()
    barrier = pltpu.get_barrier_semaphore()
    for d in range(1, m):
        pl.semaphore_signal(barrier, inc=1, device_id={"tp": tp_at[d]}, device_id_type=MESH)
    for k in range(1, n):
        pl.semaphore_signal(barrier, inc=1, device_id={"ep": ep_up[k]}, device_id_type=MESH)
    pl.semaphore_wait(barrier, m - 1 + n - 1)

    heads = []
    for d in range(1, m):
        copy = remote(head_ref, head_all.at[tp], head_send.at[d], head_recv.at[d], {"tp": tp_at[d]})
        copy.start()
        heads.append(copy)
    for load in loads[1:]:
        load.start()
    head_all[tp] = head_ref[...]
    loads[0].wait()
    for copy in heads:
        copy.wait_recv()
    mixed = jnp.zeros((rows, width), F32)
    for j in range(m):
        mixed += jnp.dot(head_all[j], mix_v[j * head_width:(j + 1) * head_width, :],
                         preferred_element_type=F32)
    residual = (tok_ref[...].astype(F32) + mixed).astype(BF16)
    resid[...] = residual
    picked = jnp.dot(disp_ref[...], residual, preferred_element_type=F32)
    outgoing[...] = picked.reshape(n, cap, width).astype(BF16)

    own = pltpu.make_async_copy(outgoing.at[me], seg.at[tp, 0], local_sem.at[0])
    own.start()
    sends = [own]
    for k in range(1, n):
        copy = remote(outgoing.at[ep_up[k]], seg.at[tp, k], disp_send.at[k], disp_recv.at[k],
                      {"ep": ep_up[k]})
        copy.start()
        sends.append(copy)
    forwards = []
    for k in range(n):
        if k == 0:
            own.wait()
        else:
            sends[k].wait_recv()
        row = []
        for d in range(1, m):
            copy = remote(seg.at[tp, k], seg.at[tp, k], fwd_send.at[d, k], fwd_recv.at[d, k],
                          {"tp": tp_at[d]})
            copy.start()
            row.append(copy)
        forwards.append(row)

    for load in loads[1:]:
        load.wait()
    parts = []
    for g in range(GROUPS):
        lo = g * per
        for k in range(lo, lo + per):
            for copy in forwards[k]:
                copy.wait_recv()
        total = jnp.zeros((group_rows, 1), F32)
        for j in range(m):
            block = seg[j, lo:lo + per].astype(F32).reshape(group_rows, width)
            total += jnp.sum(block * block, axis=1, keepdims=True)
        scale = lax.rsqrt(total / (m * width) + EPS)
        for j in range(m):
            block = seg[j, lo:lo + per].astype(F32).reshape(group_rows, width)
            normed[:, j * width:(j + 1) * width] = (
                block * scale * gain_ref[j:j + 1, :]).astype(BF16)

        def hidden_tile(c, carry):
            cols = pl.ds(pl.multiple_of(c * 256, 256), 256)
            gate = jnp.dot(normed[...], gate_v[:, cols], preferred_element_type=F32)
            up = jnp.dot(normed[...], up_v[:, cols], preferred_element_type=F32)
            hidden[:, cols] = (jax.nn.silu(gate) * up).astype(BF16)
            return carry

        lax.fori_loop(0, gate_v.shape[1] // 256, hidden_tile, 0)
        row = []
        for d in list(range(1, m)) + [0]:
            cols = pl.ds(pl.multiple_of(tp_at[d] * width, width), width)
            part[d, g] = jnp.dot(hidden[...], down_v[:, cols],
                                 preferred_element_type=F32).astype(BF16)
            if d > 0:
                copy = remote(part.at[d, g], arrived.at[d, g], part_send.at[d, g],
                              part_recv.at[d, g], {"tp": tp_at[d]})
                copy.start()
                row.append(copy)
        parts.append(row)

    backs = []
    for g in range(GROUPS):
        for copy in parts[g]:
            copy.wait_recv()
        total = part[0, g].astype(F32)
        for d in range(1, m):
            total += arrived[d, g].astype(F32)
        lo = g * per
        result[lo:lo + per] = total.reshape(per, cap, width).astype(BF16)
        for k in range(lo, lo + per):
            if k == 0:
                copy = pltpu.make_async_copy(result.at[0], returned.at[me], local_sem.at[1])
            else:
                copy = remote(result.at[k], returned.at[me], back_send.at[k], back_recv.at[k],
                              {"ep": ep_down[k]})
            copy.start()
            backs.append(copy)
    backs[0].wait()
    for copy in backs[1:]:
        copy.wait_recv()
    slots = returned[...].astype(F32).reshape(n * cap, width).astype(BF16)
    total = resid[...].astype(F32)
    for j in range(weight_ref.shape[1]):
        pair = jnp.dot(comb_ref[j * rows:(j + 1) * rows, :], slots, preferred_element_type=F32)
        total += weight_ref[:, j:j + 1] * pair
    out_ref[...] = total.astype(BF16)
    for copy in heads:
        copy.wait_send()
    for copy in sends[1:]:
        copy.wait_send()
    for row in forwards + parts:
        for copy in row:
            copy.wait_send()
    for copy in backs[1:]:
        copy.wait_send()


def layer_tail(n, m, cap, head_out, tokens, gain, dispatch, combine, weights, w_mix, w_gate, w_up,
               w_down):
    rows, width = tokens.shape
    hidden_width = w_gate.shape[2]
    half = n // GROUPS * cap
    vmem = pl.BlockSpec(memory_space=pltpu.VMEM)
    hbm = pl.BlockSpec(memory_space=pl.ANY)
    dma = pltpu.SemaphoreType.DMA
    return pl.pallas_call(
        functools.partial(tail_kernel, n, m),
        out_shape=jax.ShapeDtypeStruct((rows, width), BF16),
        in_specs=[vmem] * 6 + [hbm] * 4,
        out_specs=vmem,
        scratch_shapes=[
            pltpu.VMEM((m,) + head_out.shape, BF16),
            pltpu.VMEM(w_mix.shape, BF16),
            pltpu.VMEM(w_gate.shape[1:], BF16),
            pltpu.VMEM(w_up.shape[1:], BF16),
            pltpu.VMEM(w_down.shape[1:], BF16),
            pltpu.VMEM((n, cap, width), BF16),
            pltpu.VMEM((m, n, cap, width), BF16),
            pltpu.VMEM((half, m * width), BF16),
            pltpu.VMEM((half, hidden_width), BF16),
            pltpu.VMEM((m, GROUPS, half, width), BF16),
            pltpu.VMEM((m, GROUPS, half, width), BF16),
            pltpu.VMEM((n, cap, width), BF16),
            pltpu.VMEM((n, cap, width), BF16),
            pltpu.VMEM((rows, width), BF16),
            dma((4,)),
            dma((m,)), dma((m,)),
            dma((n,)), dma((n,)),
            dma((m, n)), dma((m, n)),
            dma((m, GROUPS)), dma((m, GROUPS)),
            dma((n,)), dma((n,)),
            dma((2,)),
        ],
        compiler_params=pltpu.CompilerParams(
            collective_id=0, has_side_effects=True, vmem_limit_bytes=40 * 1024 * 1024),
        name="layer_tail",
    )(head_out, tokens, gain, dispatch, combine, weights, w_mix, w_gate, w_up, w_down)


def shards(
    tokens,
    state,
    attn_gain,
    ffn_gain,
    w_query,
    w_key,
    w_value,
    w_output_gate,
    w_decay,
    w_beta,
    decay_rate,
    decay_shift,
    head_gain,
    w_mix_out,
    expert_ids,
    expert_weights,
    w_gate,
    w_up,
    w_down,
):
    groups = lax.axis_size("ep")
    members = lax.axis_size("tp")
    seq_count = tokens.shape[0]
    own_width = tokens.shape[1]
    head_dim = head_gain.shape[0]
    heads_here = decay_rate.shape[0]
    top_count = expert_ids.shape[1]
    assert w_gate.shape[0] == 1
    capacity = max(2, 2 * seq_count * top_count // groups)
    whole_rows = lax.all_gather(tokens, "tp", axis=1, tiled=True)
    whole_f32 = whole_rows.astype(jnp.float32)
    normed = (
        whole_f32
        * lax.rsqrt(jnp.mean(whole_f32 * whole_f32, axis=1, keepdims=True) + EPS)
        * attn_gain
    ).astype(jnp.bfloat16)

    def project(weight):
        return jnp.dot(normed, weight, preferred_element_type=jnp.float32)

    def by_head(values):
        return values.reshape(seq_count, heads_here, head_dim)

    first_head = lax.axis_index("tp") * heads_here
    decay_cols = lax.dynamic_slice_in_dim(w_decay, first_head, heads_here, 1)
    beta_cols = lax.dynamic_slice_in_dim(w_beta, first_head, heads_here, 1)
    query_proj = stored(project(w_query))
    key_proj = stored(project(w_key))
    value_proj = stored(project(w_value))
    gate_proj = stored(project(w_output_gate))
    keep_rate = jnp.exp(-decay_rate * jax.nn.softplus(project(decay_cols) + decay_shift))
    beta_gate = jax.nn.sigmoid(project(beta_cols))
    query_head = unit_norm(jax.nn.silu(by_head(query_proj))) * head_dim ** (-0.5)
    key_head = unit_norm(jax.nn.silu(by_head(key_proj)))
    value_head = jax.nn.silu(by_head(value_proj))
    decayed = keep_rate[:, :, None, None] * state
    recalled = jnp.einsum("thd,thde->the", key_head, decayed, precision=lax.Precision.HIGHEST)
    correction = beta_gate[:, :, None] * (value_head - recalled)
    new_state = decayed + key_head[:, :, :, None] * correction[:, :, None, :]
    reading = jnp.einsum("thd,thde->the", query_head, new_state, precision=lax.Precision.HIGHEST)
    reading_scale = lax.rsqrt(jnp.mean(reading * reading, axis=-1, keepdims=True) + EPS)
    head_out = (reading * reading_scale * head_gain * jax.nn.silu(by_head(gate_proj))).astype(
        jnp.bfloat16
    )
    head_out = head_out.reshape(seq_count, heads_here * head_dim)

    flat_ids = expert_ids.reshape(seq_count * top_count)
    one_hot = (flat_ids[:, None] == jnp.arange(groups, dtype=jnp.int32)[None, :]).astype(jnp.int32)
    pair_index = jnp.arange(seq_count * top_count, dtype=jnp.int32)
    lower_mask = (pair_index[:, None] > pair_index[None, :]).astype(jnp.int32)
    earlier = jnp.dot(lower_mask, one_hot)
    slot_rank = jnp.sum(earlier * one_hot, axis=1)
    slot_of = (flat_ids * capacity + slot_rank).reshape(seq_count, top_count)
    slot_index = jnp.arange(groups * capacity, dtype=jnp.int32)
    dispatch = jnp.any(slot_index[:, None, None] == slot_of[None, :, :], axis=2).astype(BF16)
    combine = (slot_of.T.reshape(-1)[:, None] == slot_index[None, :]).astype(BF16)
    layer_out = layer_tail(
        groups, members, capacity, head_out, tokens, ffn_gain.reshape(members, own_width),
        dispatch, combine, expert_weights, w_mix_out, w_gate, w_up, w_down)
    return (layer_out, new_state)


def solution(mesh):
    in_specs = (
        P("ep", "tp"),
        P("ep", "tp", None, None),
        P(),
        P(),
        P(None, "tp"),
        P(None, "tp"),
        P(None, "tp"),
        P(None, "tp"),
        P(),
        P(),
        P("tp"),
        P("tp"),
        P(),
        P(None, "tp"),
        P("ep", None),
        P("ep", None),
        P("ep", None, "tp"),
        P("ep", None, "tp"),
        P("ep", "tp", None),
    )
    out_specs = (P("ep", "tp"), P("ep", "tp", None, None))
    return jax.shard_map(shards, mesh=mesh, in_specs=in_specs, out_specs=out_specs, check_vma=False)
```

```python
import functools

import jax
import jax.numpy as jnp
from jax import lax
from jax.experimental import pallas as pl
from jax.experimental.pallas import tpu as pltpu
from jax.sharding import PartitionSpec as P

EPS = 1e-06
MESH = pl.DeviceIdType.MESH
GROUPS = 2
F32 = jnp.float32
BF16 = jnp.bfloat16


def remote(src, dst, send_sem, recv_sem, where):
    return pltpu.make_async_remote_copy(
        src_ref=src, dst_ref=dst, send_sem=send_sem, recv_sem=recv_sem,
        device_id=where, device_id_type=MESH)


def tail_kernel(
    n, m,
    head_ref, tok_ref, gain_ref, disp_ref, comb_ref, weight_ref,
    mix_hbm, gate_hbm, up_hbm, down_hbm,
    out_ref,
    head_all, mix_v, gate_v, up_v, down_v, outgoing, seg, normed, hidden, part,
    arrived, result, returned, resid,
    load_sem, head_send, head_recv, disp_send, disp_recv, fwd_send, fwd_recv,
    part_send, part_recv, back_send, back_recv, local_sem,
):
    me = lax.axis_index("ep")
    tp = lax.axis_index("tp")
    cap, width = outgoing.shape[1:]
    rows = tok_ref.shape[0]
    head_width = head_ref.shape[1]
    per = n // GROUPS
    group_rows = per * cap
    tp_at = [lax.rem(tp + d, m) for d in range(m)]
    ep_up = [lax.rem(me + k, n) for k in range(n)]
    ep_down = [lax.rem(me + n - k, n) for k in range(n)]

    loads = [
        pltpu.make_async_copy(mix_hbm, mix_v, load_sem.at[0]),
        pltpu.make_async_copy(gate_hbm.at[0], gate_v, load_sem.at[1]),
        pltpu.make_async_copy(up_hbm.at[0], up_v, load_sem.at[2]),
        pltpu.make_async_copy(down_hbm.at[0], down_v, load_sem.at[3]),
    ]
    loads[0].start()
    barrier = pltpu.get_barrier_semaphore()
    for d in range(1, m):
        pl.semaphore_signal(barrier, inc=1, device_id={"tp": tp_at[d]}, device_id_type=MESH)
    for k in range(1, n):
        pl.semaphore_signal(barrier, inc=1, device_id={"ep": ep_up[k]}, device_id_type=MESH)
    pl.semaphore_wait(barrier, m - 1 + n - 1)

    heads = []
    for d in range(1, m):
        copy = remote(head_ref, head_all.at[tp], head_send.at[d], head_recv.at[d], {"tp": tp_at[d]})
        copy.start()
        heads.append(copy)
    for load in loads[1:]:
        load.start()
    head_all[tp] = head_ref[...]
    loads[0].wait()
    for copy in heads:
        copy.wait_recv()
    mixed = jnp.zeros((rows, width), F32)
    for j in range(m):
        mixed += jnp.dot(head_all[j], mix_v[j * head_width:(j + 1) * head_width, :],
                         preferred_element_type=F32)
    residual = (tok_ref[...].astype(F32) + mixed).astype(BF16)
    resid[...] = residual
    picked = jnp.dot(disp_ref[...], residual, preferred_element_type=F32)
    outgoing[...] = picked.reshape(n, cap, width).astype(BF16)

    own = pltpu.make_async_copy(outgoing.at[me], seg.at[tp, 0], local_sem.at[0])
    own.start()
    sends = [own]
    for k in range(1, n):
        copy = remote(outgoing.at[ep_up[k]], seg.at[tp, k], disp_send.at[k], disp_recv.at[k],
                      {"ep": ep_up[k]})
        copy.start()
        sends.append(copy)
    forwards = []
    for k in range(n):
        if k == 0:
            own.wait()
        else:
            sends[k].wait_recv()
        row = []
        for d in range(1, m):
            copy = remote(seg.at[tp, k], seg.at[tp, k], fwd_send.at[d, k], fwd_recv.at[d, k],
                          {"tp": tp_at[d]})
            copy.start()
            row.append(copy)
        forwards.append(row)

    for load in loads[1:]:
        load.wait()
    parts = []
    for g in range(GROUPS):
        lo = g * per
        for k in range(lo, lo + per):
            for copy in forwards[k]:
                copy.wait_recv()
        total = jnp.zeros((group_rows, 1), F32)
        for j in range(m):
            block = seg[j, lo:lo + per].astype(F32).reshape(group_rows, width)
            total += jnp.sum(block * block, axis=1, keepdims=True)
        scale = lax.rsqrt(total / (m * width) + EPS)
        for j in range(m):
            block = seg[j, lo:lo + per].astype(F32).reshape(group_rows, width)
            normed[:, j * width:(j + 1) * width] = (
                block * scale * gain_ref[j:j + 1, :]).astype(BF16)

        def hidden_tile(c, carry):
            cols = pl.ds(pl.multiple_of(c * 256, 256), 256)
            gate = jnp.dot(normed[...], gate_v[:, cols], preferred_element_type=F32)
            up = jnp.dot(normed[...], up_v[:, cols], preferred_element_type=F32)
            hidden[:, cols] = (jax.nn.silu(gate) * up).astype(BF16)
            return carry

        lax.fori_loop(0, gate_v.shape[1] // 256, hidden_tile, 0)
        row = []
        for d in list(range(1, m)) + [0]:
            cols = pl.ds(pl.multiple_of(tp_at[d] * width, width), width)
            part[d, g] = jnp.dot(hidden[...], down_v[:, cols],
                                 preferred_element_type=F32).astype(BF16)
            if d > 0:
                copy = remote(part.at[d, g], arrived.at[d, g], part_send.at[d, g],
                              part_recv.at[d, g], {"tp": tp_at[d]})
                copy.start()
                row.append(copy)
        parts.append(row)

    backs = []
    for g in range(GROUPS):
        for copy in parts[g]:
            copy.wait_recv()
        total = part[0, g].astype(F32)
        for d in range(1, m):
            total += arrived[d, g].astype(F32)
        lo = g * per
        result[lo:lo + per] = total.reshape(per, cap, width).astype(BF16)
        for k in range(lo, lo + per):
            if k == 0:
                copy = pltpu.make_async_copy(result.at[0], returned.at[me], local_sem.at[1])
            else:
                copy = remote(result.at[k], returned.at[me], back_send.at[k], back_recv.at[k],
                              {"ep": ep_down[k]})
            copy.start()
            backs.append(copy)
    backs[0].wait()
    for copy in backs[1:]:
        copy.wait_recv()
    slots = returned[...].astype(F32).reshape(n * cap, width).astype(BF16)
    total = resid[...].astype(F32)
    for j in range(weight_ref.shape[1]):
        pair = jnp.dot(comb_ref[j * rows:(j + 1) * rows, :], slots, preferred_element_type=F32)
        total += weight_ref[:, j:j + 1] * pair
    out_ref[...] = total.astype(BF16)
    for copy in heads:
        copy.wait_send()
    for copy in sends[1:]:
        copy.wait_send()
    for row in forwards + parts:
        for copy in row:
            copy.wait_send()
    for copy in backs[1:]:
        copy.wait_send()


def layer_tail(n, m, cap, head_out, tokens, gain, dispatch, combine, weights, w_mix, w_gate, w_up,
               w_down):
    rows, width = tokens.shape
    hidden_width = w_gate.shape[2]
    half = n // GROUPS * cap
    vmem = pl.BlockSpec(memory_space=pltpu.VMEM)
    hbm = pl.BlockSpec(memory_space=pl.ANY)
    dma = pltpu.SemaphoreType.DMA
    return pl.pallas_call(
        functools.partial(tail_kernel, n, m),
        out_shape=jax.ShapeDtypeStruct((rows, width), BF16),
        in_specs=[vmem] * 6 + [hbm] * 4,
        out_specs=vmem,
        scratch_shapes=[
            pltpu.VMEM((m,) + head_out.shape, BF16),
            pltpu.VMEM(w_mix.shape, BF16),
            pltpu.VMEM(w_gate.shape[1:], BF16),
            pltpu.VMEM(w_up.shape[1:], BF16),
            pltpu.VMEM(w_down.shape[1:], BF16),
            pltpu.VMEM((n, cap, width), BF16),
            pltpu.VMEM((m, n, cap, width), BF16),
            pltpu.VMEM((half, m * width), BF16),
            pltpu.VMEM((half, hidden_width), BF16),
            pltpu.VMEM((m, GROUPS, half, width), BF16),
            pltpu.VMEM((m, GROUPS, half, width), BF16),
            pltpu.VMEM((n, cap, width), BF16),
            pltpu.VMEM((n, cap, width), BF16),
            pltpu.VMEM((rows, width), BF16),
            dma((4,)),
            dma((m,)), dma((m,)),
            dma((n,)), dma((n,)),
            dma((m, n)), dma((m, n)),
            dma((m, GROUPS)), dma((m, GROUPS)),
            dma((n,)), dma((n,)),
            dma((2,)),
        ],
        compiler_params=pltpu.CompilerParams(
            collective_id=0, has_side_effects=True, vmem_limit_bytes=60 * 1024 * 1024),
        name="layer_tail",
    )(head_out, tokens, gain, dispatch, combine, weights, w_mix, w_gate, w_up, w_down)


def gather_kernel(m, tok_ref, out_ref, send_sem, recv_sem):
    tp = lax.axis_index("tp")
    tp_at = [lax.rem(tp + d, m) for d in range(m)]
    barrier = pltpu.get_barrier_semaphore()
    for d in range(1, m):
        pl.semaphore_signal(barrier, inc=1, device_id={"tp": tp_at[d]}, device_id_type=MESH)
    pl.semaphore_wait(barrier, m - 1)
    copies = []
    for d in range(1, m):
        copy = remote(tok_ref, out_ref.at[tp], send_sem.at[d], recv_sem.at[d], {"tp": tp_at[d]})
        copy.start()
        copies.append(copy)
    out_ref[tp] = tok_ref[...]
    for copy in copies:
        copy.wait()


def gather_tokens(m, tokens):
    vmem = pl.BlockSpec(memory_space=pltpu.VMEM)
    return pl.pallas_call(
        functools.partial(gather_kernel, m),
        out_shape=jax.ShapeDtypeStruct((m,) + tokens.shape, BF16),
        in_specs=[vmem],
        out_specs=vmem,
        scratch_shapes=[pltpu.SemaphoreType.DMA((m,)), pltpu.SemaphoreType.DMA((m,))],
        compiler_params=pltpu.CompilerParams(collective_id=1, has_side_effects=True),
        name="gather_tokens",
    )(tokens)


def unit_norm(values):
    return values * lax.rsqrt(jnp.sum(values * values, axis=-1, keepdims=True) + EPS)


def delta_kernel(
    m, slots, cap, block,
    rate_ref, shift_ref, rows_ref, gain_ref, wq_ref, wk_ref, wv_ref, wg_ref, wd_ref, wb_ref,
    head_gain_ref, ids_ref, state_ref,
    new_ref, head_ref, disp_ref, comb_ref,
    q_s, k_s, v_s, gate_s, keep_s, beta_s, read_s,
):
    step = pl.program_id(0)
    rows, width = rows_ref.shape[1:]
    heads, dim = q_s.shape[0], q_s.shape[2]
    tp = lax.axis_index("tp")

    @pl.when(step == 0)
    def _():
        total = jnp.zeros((rows, 1), F32)
        for j in range(m):
            piece = rows_ref[j].astype(F32)
            total += jnp.sum(piece * piece, axis=1, keepdims=True)
        scale = lax.rsqrt(total / (m * width) + EPS)
        normed = [(rows_ref[j].astype(F32) * scale * gain_ref[j:j + 1, :]).astype(BF16)
                  for j in range(m)]

        def project(w_ref):
            acc = jnp.dot(normed[0], w_ref[0:width, :], preferred_element_type=F32)
            for j in range(1, m):
                acc += jnp.dot(normed[j], w_ref[j * width:(j + 1) * width, :],
                               preferred_element_type=F32)
            return acc

        def project_cols(w_ref):
            acc = jnp.zeros((rows, w_ref.shape[0]), F32)
            for j in range(m):
                acc += lax.dot_general(normed[j], w_ref[:, j * width:(j + 1) * width],
                                       (((1,), (1,)), ((), ())), preferred_element_type=F32)
            return acc

        def rounded(values):
            return values.astype(BF16).astype(F32)

        query = jax.nn.silu(rounded(project(wq_ref)))
        key = jax.nn.silu(rounded(project(wk_ref)))
        value = jax.nn.silu(rounded(project(wv_ref)))
        gate = jax.nn.silu(rounded(project(wg_ref)))
        decay_in = project_cols(wd_ref)
        beta_in = project_cols(wb_ref)
        column = lax.broadcasted_iota(jnp.int32, decay_in.shape, 1)
        for h in range(heads):
            cols = slice(h * dim, (h + 1) * dim)
            q_s[h] = unit_norm(query[:, cols]) * dim ** (-0.5)
            k_s[h] = unit_norm(key[:, cols])
            v_s[h] = value[:, cols]
            gate_s[h] = gate[:, cols]
            mine = column == tp * heads + h
            own_decay = jnp.sum(jnp.where(mine, decay_in, 0.0), axis=1, keepdims=True) + shift_ref[h]
            soft = jnp.maximum(own_decay, 0.0) + jnp.log1p(jnp.exp(-jnp.abs(own_decay)))
            keep_s[h] = jnp.broadcast_to(jnp.exp(-rate_ref[h] * soft), (rows, dim))
            own_beta = jnp.sum(jnp.where(mine, beta_in, 0.0), axis=1, keepdims=True)
            beta_s[h] = jnp.broadcast_to(jax.nn.sigmoid(own_beta), (rows, dim))

        top = ids_ref.shape[1]
        experts = slots // cap
        expert = lax.broadcasted_iota(jnp.int32, (rows, experts), 1)
        hot = [(ids_ref[:, j:j + 1] == expert).astype(F32) for j in range(top)]
        every = hot[0]
        for j in range(1, top):
            every = every + hot[j]
        lower = (lax.broadcasted_iota(jnp.int32, (rows, rows), 0)
                 > lax.broadcasted_iota(jnp.int32, (rows, rows), 1)).astype(BF16)
        earlier = jnp.dot(lower, every.astype(BF16), preferred_element_type=F32)
        slot = lax.broadcasted_iota(jnp.int32, (rows, slots), 1)
        used = jnp.zeros((rows, slots), F32)
        for j in range(top):
            rank = jnp.sum(earlier * hot[j], axis=1, keepdims=True).astype(jnp.int32)
            hit = (slot == ids_ref[:, j:j + 1] * cap + rank).astype(F32)
            comb_ref[j * rows:(j + 1) * rows, :] = hit.astype(BF16)
            used = used + hit
            earlier = earlier + hot[j]
        disp_ref[...] = used.T.astype(BF16)

    here = pl.ds(pl.multiple_of(step * block, block), block)
    for h in range(heads):
        key = k_s[h, here, :]
        query = q_s[h, here, :]
        decayed = state_ref[:, h] * keep_s[h, here, :][:, None, :]
        key_col = jnp.broadcast_to(key[:, :, None], decayed.shape)
        recalled = jnp.sum(key_col * decayed, axis=1)
        correction = beta_s[h, here, :] * (v_s[h, here, :] - recalled)
        updated = decayed + key_col * correction[:, None, :]
        new_ref[:, h] = updated
        read_s[h, here, :] = jnp.sum(query[:, :, None] * updated, axis=1)

    @pl.when(step == pl.num_programs(0) - 1)
    def _():
        outs = []
        for h in range(heads):
            reading = read_s[h]
            scale = lax.rsqrt(jnp.mean(reading * reading, axis=-1, keepdims=True) + EPS)
            outs.append(reading * scale * head_gain_ref[...] * gate_s[h])
        head_ref[...] = (jnp.concatenate(outs, axis=1) if heads > 1 else outs[0]).astype(BF16)


def delta_step(m, slots, cap, gathered, gain, w_query, w_key, w_value, w_output_gate, w_decay,
               w_beta, rate, shift, head_gain, ids, state):
    rows, heads, dim = state.shape[:3]
    block = 8
    smem = pl.BlockSpec(memory_space=pltpu.SMEM)
    vmem = pl.BlockSpec(memory_space=pltpu.VMEM)
    spec = pl.BlockSpec((block,) + state.shape[1:], lambda i: (i, 0, 0, 0))
    per_head = pltpu.VMEM((heads, rows, dim), F32)
    pairs = rows * ids.shape[1]
    return pl.pallas_call(
        functools.partial(delta_kernel, m, slots, cap, block),
        grid=(rows // block,),
        out_shape=(
            jax.ShapeDtypeStruct(state.shape, F32),
            jax.ShapeDtypeStruct((rows, heads * dim), BF16),
            jax.ShapeDtypeStruct((slots, rows), BF16),
            jax.ShapeDtypeStruct((pairs, slots), BF16),
        ),
        in_specs=[smem, smem] + [vmem] * 10 + [spec],
        out_specs=(spec, vmem, vmem, vmem),
        scratch_shapes=[per_head] * 7,
        compiler_params=pltpu.CompilerParams(vmem_limit_bytes=40 * 1024 * 1024),
        name="delta_step",
    )(rate, shift, gathered, gain, w_query, w_key, w_value, w_output_gate, w_decay.T, w_beta.T,
      head_gain, ids, state)


def shards(
    tokens,
    state,
    attn_gain,
    ffn_gain,
    w_query,
    w_key,
    w_value,
    w_output_gate,
    w_decay,
    w_beta,
    decay_rate,
    decay_shift,
    head_gain,
    w_mix_out,
    expert_ids,
    expert_weights,
    w_gate,
    w_up,
    w_down,
):
    groups = lax.axis_size("ep")
    members = lax.axis_size("tp")
    seq_count = tokens.shape[0]
    own_width = tokens.shape[1]
    top_count = expert_ids.shape[1]
    assert w_gate.shape[0] == 1
    capacity = max(2, 2 * seq_count * top_count // groups)
    gathered = gather_tokens(members, tokens)
    new_state, head_out, dispatch, combine = delta_step(
        members, groups * capacity, capacity, gathered, attn_gain.reshape(members, own_width),
        w_query, w_key, w_value, w_output_gate, w_decay, w_beta, decay_rate, decay_shift,
        head_gain[None, :], expert_ids, state)
    layer_out = layer_tail(
        groups, members, capacity, head_out, tokens, ffn_gain.reshape(members, own_width),
        dispatch, combine, expert_weights, w_mix_out, w_gate, w_up, w_down)
    return (layer_out, new_state)


def solution(mesh):
    in_specs = (
        P("ep", "tp"),
        P("ep", "tp", None, None),
        P(),
        P(),
        P(None, "tp"),
        P(None, "tp"),
        P(None, "tp"),
        P(None, "tp"),
        P(),
        P(),
        P("tp"),
        P("tp"),
        P(),
        P(None, "tp"),
        P("ep", None),
        P("ep", None),
        P("ep", None, "tp"),
        P("ep", None, "tp"),
        P("ep", "tp", None),
    )
    out_specs = (P("ep", "tp"), P("ep", "tp", None, None))
    return jax.shard_map(shards, mesh=mesh, in_specs=in_specs, out_specs=out_specs, check_vma=False)
```
